32 devices in a mesh: sp: 4 (over z), fs: 4 (over y, x), tp: 2 (over core).
Axes of the slice: x: 2, y: 2, z: 4, core: 2. Of those that a mesh axis runs over, the one named last changes fastest.
Arguments:
- tokens: bfloat16 [4, 4096, 2048], P('fs', ('sp', 'tp')), may hold values from -6 to 6
- norm_gain: bfloat16 [2048], replicated, may hold values from 0.099609375 to 1.8984375
- w_query: bfloat16 [2048, 1024], P(None, 'tp'), may hold values from -0.125 to 0.125
- w_key: bfloat16 [2048, 1024], P(None, 'tp'), may hold values from -0.125 to 0.125
- w_value: bfloat16 [2048, 1024], P(None, 'tp'), may hold values from -0.125 to 0.125
- w_outgate: bfloat16 [2048, 1024], P(None, 'tp'), may hold values from -0.125 to 0.125
- w_gatein: bfloat16 [2048, 1024], P(None, 'tp'), may hold values from -0.125 to 0.125
- w_gateout: bfloat16 [2048, 1024], P(None, 'tp'), may hold values from -0.125 to 0.125
- w_convin: bfloat16 [2048, 1024], P(None, 'tp'), may hold values from -0.125 to 0.125
- w_igate: bfloat16 [2048, 8], replicated, may hold values from -0.125 to 0.125
- w_fgate: bfloat16 [2048, 8], replicated, may hold values from -0.125 to 0.125
- input_bias: float32 [8], replicated, may hold values from -1 to 101
- forget_bias: float32 [8], replicated
- forget_extra: float32 [4, 4096, 8], P('fs', 'sp', 'tp'), may hold values from -0.7 to 0
- init_memory: float32 [4, 8, 128, 128], P('fs', 'tp'), may hold values from -56 to 56
- head_gain: bfloat16 [1024], replicated, may hold values from 0.099609375 to 1.8984375
- conv_taps: bfloat16 [3, 1024], replicated, may hold values from -3.5 to 3.5
- out_memory: bfloat16 [1024, 2048], P('tp'), may hold values from -0.125 to 0.125
- out_conv: bfloat16 [1024, 2048], P('tp'), may hold values from -0.125 to 0.125
Outputs:
- layer_out: bfloat16 [4, 4096, 2048], P('fs', ('sp', 'tp'))
The draws below stay inside these ranges and needn't reach their ends.
All inputs are finite; a program needn't handle non-finite values.
Results may differ from the reference program's by a relative error of at most 0.017.
Values may be sent and summed in bfloat16 or wider, within the bound.
A program may use at most 128 MiB of HBM per device.

```python
import math
import jax
import jax.numpy as jnp
from jax import lax

D = 2048
MEMORY_HEADS = 8
DH = 128
HALF = 1024
BLOCK = 128
TAPS = 3
TOK_DEV = 1024
SEQUENCE_COUNT = 4
SEQUENCE_LENGTH = 4096
N_TP = 2


def draw_input_bias(key, part):
    base_key = jax.random.fold_in(jax.random.fold_in(key, 11), 0)
    steady_forget = jax.random.uniform(base_key, (MEMORY_HEADS,), jnp.float32, -1.0, 1.0)
    return steady_forget


def draw_forget_bias(key, part):
    slow_key, fast_key, pick_key = jax.random.split(jax.random.fold_in(key, 23), 3)
    slow_bias = math.log(SEQUENCE_LENGTH) + jax.random.uniform(slow_key, (MEMORY_HEADS,), jnp.float32, 1.5, 3.0)
    fast_bias = jax.random.uniform(fast_key, (MEMORY_HEADS,), jnp.float32, 3.4, 4.6)
    chosen = jax.random.permutation(pick_key, MEMORY_HEADS) < MEMORY_HEADS // 2
    return jnp.where(chosen, fast_bias, slow_bias)


def draw_forget_extra(key, part):
    rate_key, place_random_key, drop_random_key = jax.random.split(jax.random.fold_in(key, 37), 3)
    span_count = SEQUENCE_LENGTH // TOK_DEV
    span_rates = jnp.exp(jax.random.uniform(rate_key, (SEQUENCE_COUNT, span_count, 1, MEMORY_HEADS), jnp.float32, math.log(0.1), math.log(0.8))) / SEQUENCE_LENGTH
    steady_forget = -jnp.broadcast_to(span_rates, (SEQUENCE_COUNT, span_count, TOK_DEV, MEMORY_HEADS)).reshape(SEQUENCE_COUNT, SEQUENCE_LENGTH, MEMORY_HEADS)
    sudden_drop_places = jax.random.randint(place_random_key, (SEQUENCE_COUNT, 2), 0, SEQUENCE_LENGTH)
    sudden_drop_mask = jnp.any(jnp.arange(SEQUENCE_LENGTH)[None, :, None] == sudden_drop_places[:, None, :], axis=-1)
    sudden_drop_values = jax.random.uniform(drop_random_key, (SEQUENCE_COUNT, SEQUENCE_LENGTH, MEMORY_HEADS), jnp.float32, math.log(0.5), math.log(0.8))
    return steady_forget + jnp.where(sudden_drop_mask[:, :, None], sudden_drop_values, 0.0)


def shard_levels(key, extent, cuts, smallest, top_value):
    level = 1.0
    for dim, parts in cuts:
        steps = jax.random.uniform(jax.random.fold_in(jax.random.fold_in(key, 6), dim), (parts,), jnp.float32, smallest / len(cuts), top_value / len(cuts))
        level = level * jnp.repeat(jnp.exp(steps), extent[dim] // parts).reshape((-1,) + (1,) * (len(extent) - 1 - dim))
    return level


def gaussian(own_key, extent, spread, reach, shards=(), held_as=jnp.bfloat16):
    result = spread * jax.random.normal(own_key, extent, jnp.float32)
    if shards:
        result = result * shard_levels(own_key, extent, shards, -0.22, 0.18)
    return jnp.clip(result, -reach, reach).astype(held_as)


def setup_inputs(seed: int = 0) -> dict:
    seeds = jax.random.split(jax.random.key(seed), 20)
    return {
        "tokens": gaussian(seeds[0], (SEQUENCE_COUNT, SEQUENCE_LENGTH, D), 1.0, 6.0, ((0, 4), (1, 8))),
        "norm_gain": jnp.clip(1.0 + 0.18 * jax.random.normal(seeds[1], (D,), jnp.float32), 0.099609375, 1.8984375).astype(jnp.bfloat16),
        "w_query": gaussian(seeds[2], (D, HALF), D ** -0.5, 0.125, ((1, 2),)),
        "w_key": gaussian(seeds[3], (D, HALF), D ** -0.5, 0.125, ((1, 2),)),
        "w_value": gaussian(seeds[4], (D, HALF), D ** -0.5, 0.125, ((1, 2),)),
        "w_outgate": gaussian(seeds[5], (D, HALF), D ** -0.5, 0.125, ((1, 2),)),
        "w_gatein": gaussian(seeds[6], (D, HALF), D ** -0.5, 0.125, ((1, 2),)),
        "w_gateout": gaussian(seeds[7], (D, HALF), D ** -0.5, 0.125, ((1, 2),)),
        "w_convin": gaussian(seeds[8], (D, HALF), D ** -0.5, 0.125, ((1, 2),)),
        "w_igate": gaussian(seeds[9], (D, MEMORY_HEADS), D ** -0.5, 0.125),
        "w_fgate": gaussian(seeds[10], (D, MEMORY_HEADS), D ** -0.5, 0.125),
        "input_bias": draw_input_bias(jax.random.fold_in(seeds[19], 71), 0),
        "forget_bias": draw_forget_bias(jax.random.fold_in(seeds[19], 71), 0),
        "forget_extra": draw_forget_extra(jax.random.fold_in(seeds[19], 71), 0),
        "init_memory": gaussian(seeds[14], (SEQUENCE_COUNT, MEMORY_HEADS, DH, DH), (0.15 * SEQUENCE_LENGTH ** 0.5), 56.0, ((0, 4), (1, 2)), jnp.float32),
        "head_gain": jnp.clip(1.0 + 0.18 * jax.random.normal(seeds[15], (HALF,), jnp.float32), 0.099609375, 1.8984375).astype(jnp.bfloat16),
        "conv_taps": gaussian(seeds[16], (TAPS, HALF), TAPS ** -0.5, 3.5),
        "out_memory": gaussian(seeds[17], (HALF, D), (2 * HALF) ** -0.5, 0.125, ((0, 2),)),
        "out_conv": gaussian(seeds[18], (HALF, D), (2 * HALF) ** -0.5, 0.125, ((0, 2),)),
    }


EPSILON = 1e-06

def memory_cell(queries, key_rows, value_rows, input_pre, log_forget, start_memory):
    nblocks = SEQUENCE_LENGTH // BLOCK
    key_factor = DH ** (-0.5)
    highest = lax.Precision.HIGHEST

    def blocked(matrix):
        return jnp.swapaxes(matrix.reshape(nblocks, BLOCK, MEMORY_HEADS, DH), 1, 2).astype(jnp.float32)

    def gate_blocks(matrix):
        return jnp.swapaxes(matrix.reshape(nblocks, BLOCK, MEMORY_HEADS), 1, 2)
    causal = jnp.tril(jnp.ones((BLOCK, BLOCK), dtype=bool))

    def advance(memory_pair, inputs):
        memory, log_scale = memory_pair
        query_blk, key_blk, value_blk, gate_in_blk, forget_blk = inputs
        cumulative = jnp.cumsum(forget_blk, axis=-1)
        block_total = cumulative[:, -1]
        exponent = block_total[:, None] - cumulative + gate_in_blk
        block_top = lax.optimization_barrier(jnp.max(exponent, axis=-1))
        weighted_keys = (jnp.exp(exponent - block_top[:, None])[:, :, None] * key_blk * key_factor).astype(jnp.bfloat16)
        weighted_keys = lax.optimization_barrier(weighted_keys).astype(jnp.float32)
        block_terms = jnp.einsum('hsd,hse->hde', weighted_keys, value_blk, precision=highest)
        pair_log = cumulative[:, :, None] - cumulative[:, None, :] + gate_in_blk[:, None, :]
        pair_log = jnp.where(causal, pair_log, -jnp.inf)
        carried_log = cumulative + log_scale[:, None]
        row_top = jnp.maximum(carried_log, lax.optimization_barrier(jnp.max(pair_log, axis=-1)))
        scores = jnp.einsum('htd,hsd->hts', query_blk, key_blk, precision=highest) * key_factor
        weighted = (jnp.exp(pair_log - row_top[:, :, None]) * scores).astype(jnp.bfloat16)
        weighted = lax.optimization_barrier(weighted).astype(jnp.float32)
        carried = jnp.einsum('htd,hde->hte', query_blk, memory, precision=highest)
        readout = jnp.exp(carried_log - row_top)[:, :, None] * carried
        readout = readout + jnp.einsum('hts,hse->hte', weighted, value_blk, precision=highest)
        new_scale = jnp.maximum(block_total + log_scale, block_top)
        new_memory = jnp.exp(block_total + log_scale - new_scale)[:, None, None] * memory
        new_memory = new_memory + jnp.exp(block_top - new_scale)[:, None, None] * block_terms
        return ((new_memory, new_scale), readout)
    start_pair = (start_memory, jnp.zeros((MEMORY_HEADS,), jnp.float32))
    inputs = (blocked(queries), blocked(key_rows), blocked(value_rows), gate_blocks(input_pre), gate_blocks(log_forget))
    final_pair, readouts = lax.scan(advance, start_pair, inputs)
    return jnp.swapaxes(readouts, 1, 2).reshape(SEQUENCE_LENGTH, HALF)

def reference(tokens, norm_gain, w_query, w_key, w_value, w_outgate, w_gatein, w_gateout, w_convin, w_igate, w_fgate, input_bias, forget_bias, forget_extra, init_memory, head_gain, conv_taps, out_memory, out_conv):
    group_width = HALF // N_TP
    outputs = []
    for seq_index in range(SEQUENCE_COUNT):
        seq_rows = tokens[seq_index].astype(jnp.float32)
        normed = seq_rows * lax.rsqrt(lax.optimization_barrier(jnp.mean(seq_rows * seq_rows, axis=-1, keepdims=True)) + EPSILON)
        normed = (normed * norm_gain.astype(jnp.float32)).astype(jnp.bfloat16)

        def project(weight):
            return jnp.dot(normed, weight, preferred_element_type=jnp.float32).astype(jnp.bfloat16)
        queries = project(w_query)
        key_rows = project(w_key)
        value_rows = project(w_value)
        out_gate = project(w_outgate)
        gate_in = project(w_gatein)
        gate_out = project(w_gateout)
        conv_input = project(w_convin)
        input_pre = jnp.dot(normed, w_igate, preferred_element_type=jnp.float32) + input_bias
        forget_pre = jnp.dot(normed, w_fgate, preferred_element_type=jnp.float32) + forget_bias
        log_forget = jax.nn.log_sigmoid(forget_pre) + forget_extra[seq_index]
        readout = memory_cell(queries, key_rows, value_rows, input_pre, log_forget, init_memory[seq_index])
        per_head = readout.reshape(SEQUENCE_LENGTH, MEMORY_HEADS, DH)
        normalized = per_head * lax.rsqrt(lax.optimization_barrier(jnp.mean(per_head * per_head, axis=-1, keepdims=True)) + EPSILON)
        memory_out = normalized.reshape(SEQUENCE_LENGTH, HALF) * head_gain.astype(jnp.float32) * jax.nn.sigmoid(out_gate.astype(jnp.float32))
        memory_out = memory_out.astype(jnp.bfloat16)
        conv_product = (gate_in.astype(jnp.float32) * conv_input.astype(jnp.float32)).astype(jnp.bfloat16)
        conv_product = lax.optimization_barrier(conv_product).astype(jnp.float32)
        padded = jnp.pad(conv_product, ((TAPS - 1, 0), (0, 0)))
        mixed_conv = jnp.zeros((SEQUENCE_LENGTH, HALF), jnp.float32)
        for tap_index in range(TAPS):
            mixed_conv = mixed_conv + padded[tap_index:tap_index + SEQUENCE_LENGTH] * conv_taps[tap_index].astype(jnp.float32)
        conv_out = (gate_out.astype(jnp.float32) * mixed_conv).astype(jnp.bfloat16)
        summed = jnp.zeros((SEQUENCE_LENGTH, D), jnp.float32)
        for part_index in range(N_TP):
            low_col = part_index * group_width
            high_col = low_col + group_width
            partial_value = jnp.dot(memory_out[:, low_col:high_col], out_memory[low_col:high_col], preferred_element_type=jnp.float32)
            partial_value = partial_value + jnp.dot(conv_out[:, low_col:high_col], out_conv[low_col:high_col], preferred_element_type=jnp.float32)
            summed = summed + lax.optimization_barrier(partial_value.astype(jnp.bfloat16)).astype(jnp.float32)
        outputs.append(summed.astype(jnp.bfloat16))
    return jnp.stack(outputs)
```

```python
import functools

import jax
import jax.numpy as jnp
from jax import lax
from jax.experimental import pallas as pl
from jax.experimental.pallas import tpu as pltpu
from jax.sharding import PartitionSpec as P

BLOCK = 128
EPSILON = 1e-06
LOWEST_LOG = -1e30
MESH = pl.DeviceIdType.MESH
F32 = jnp.float32
BF16 = jnp.bfloat16
PAD = 8
RIM = 16
NORM_ROWS = 64
OUT_COLS = 512

KEY, VALUE, GATE_IN, CONV_IN, GATE_OUT, QUERY, OUT_GATE = range(7)


def kernel(
    n_sp,
    tokens,
    norm_gain,
    w_key,
    w_value,
    w_gatein,
    w_convin,
    w_gateout,
    w_query,
    w_outgate,
    gate_w,
    gate_bias,
    extra,
    init_memory,
    head_gain,
    conv_taps,
    out_memory,
    out_conv,
    layer_out,
    tok,
    normed,
    weights,
    out_w,
    proj,
    gate_pre,
    row_log,
    col_log,
    block_sum,
    block_peak,
    terms,
    running,
    running_log,
    starts,
    starts_log,
    seg_memory,
    seg_log,
    got_memory,
    got_log,
    conv_rows,
    rim,
    mix,
    part_send,
    part_got,
    result,
    local_sem,
    weight_sem,
    out_sem,
    token_sem,
    seg_send,
    seg_recv,
    rim_sem,
    part_sem_send,
    part_sem_recv,
):
    me = lax.axis_index("tp")
    other = 1 - me
    place = lax.axis_index("sp")
    half = tok.shape[1]
    total_rows = normed.shape[0]
    width = w_key.shape[1]
    heads = init_memory.shape[0]
    dh = init_memory.shape[1]
    nblocks = total_rows // BLOCK
    key_factor = dh ** (-0.5)
    out_width = layer_out.shape[1]
    n_out = out_width // OUT_COLS

    barrier = pltpu.get_barrier_semaphore()
    pl.semaphore_signal(barrier, inc=1, device_id={"tp": other}, device_id_type=MESH)
    for d in range(1, n_sp):
        pl.semaphore_signal(
            barrier, inc=1, device_id={"sp": lax.rem(place + d, n_sp)}, device_id_type=MESH
        )

    own_copy = pltpu.make_async_copy(tokens, tok.at[0], local_sem.at[0])
    own_copy.start()
    w_in = (w_key, w_value, w_gatein, w_convin, w_gateout, w_query, w_outgate)
    w_copies = [
        pltpu.make_async_copy(w, weights.at[s], weight_sem.at[s]) for s, w in enumerate(w_in)
    ]
    out_copies = [
        pltpu.make_async_copy(out_memory, out_w.at[pl.ds(0, width)], weight_sem.at[7]),
        pltpu.make_async_copy(out_conv, out_w.at[pl.ds(width, width)], weight_sem.at[8]),
    ]
    for c in w_copies + out_copies:
        c.start()

    pl.semaphore_wait(barrier, n_sp)
    token_copy = pltpu.make_async_remote_copy(
        src_ref=tokens,
        dst_ref=tok.at[1],
        send_sem=token_sem.at[0],
        recv_sem=token_sem.at[1],
        device_id={"tp": other},
        device_id_type=MESH,
    )
    token_copy.start()
    own_copy.wait()

    def rows_of(index, size):
        return pl.ds(pl.multiple_of(index * size, size), size)

    def normalize(slot, base):
        @pl.loop(0, half // NORM_ROWS)
        def _(c):
            x = tok[slot, rows_of(c, NORM_ROWS), :].astype(F32)
            scale = lax.rsqrt(jnp.mean(x * x, axis=-1, keepdims=True) + EPSILON)
            y = (x * scale) * norm_gain[...].astype(F32)
            normed[pl.ds(pl.multiple_of(base + c * NORM_ROWS, NORM_ROWS), NORM_ROWS), :] = y.astype(
                BF16
            )

    def project(slot, rows):
        proj[slot, rows, :] = jnp.dot(
            normed[rows, :], weights[slot], preferred_element_type=F32
        ).astype(BF16)

    @pl.loop(0, 2)
    def _(step):
        index = lax.rem(me + step, 2)

        @pl.when(step == 1)
        def _():
            token_copy.wait_recv()

        normalize(step, index * half)
        rows = rows_of(index, half)
        gate_pre[rows, :] = jnp.dot(normed[rows, :], gate_w[...], preferred_element_type=F32)

        @pl.loop(KEY, VALUE + 1)
        def _(slot):
            @pl.when(step == 0)
            def _():
                pltpu.make_async_copy(w_key, weights.at[slot], weight_sem.at[slot]).wait()

            project(slot, rows)

    row_i = lax.broadcasted_iota(jnp.int32, (BLOCK, BLOCK), 0)
    col_i = lax.broadcasted_iota(jnp.int32, (BLOCK, BLOCK), 1)
    upper = jnp.where(row_i <= col_i, 1.0, 0.0).astype(F32)
    for h in range(heads):
        running[h] = jnp.zeros((dh, dh), F32)
    running_log[0:PAD] = jnp.full((PAD, BLOCK), LOWEST_LOG, F32)
    running_log[PAD : 2 * PAD] = jnp.zeros((PAD, BLOCK), F32)

    def head_cols(h):
        return slice(h * dh, (h + 1) * dh)

    @pl.loop(0, nblocks)
    def _(b):
        rows = rows_of(b, BLOCK)
        pre = jnp.transpose(gate_pre[rows, :])
        v = pre[0:PAD] + gate_bias[0:PAD]
        log_forget = jnp.minimum(v, 0.0) - jnp.log1p(jnp.exp(-jnp.abs(v))) + extra[:, rows]
        gate_in = pre[PAD : 2 * PAD] + gate_bias[PAD : 2 * PAD]
        cumulative = jnp.dot(
            log_forget, upper, precision=lax.Precision.HIGHEST, preferred_element_type=F32
        )
        total = cumulative[:, BLOCK - 1 : BLOCK]
        exponent = total - cumulative + gate_in
        peak = jnp.max(exponent, axis=1, keepdims=True)
        key_weight = jnp.exp(exponent - peak)
        row_log[b, 0:PAD] = cumulative
        row_log[b, PAD : 2 * PAD] = gate_in
        stacked = jnp.concatenate(
            [cumulative, key_weight, jnp.zeros((BLOCK - 2 * PAD, BLOCK), F32)], axis=0
        )
        columns = jnp.transpose(stacked)
        col_log[b] = columns
        total = jnp.broadcast_to(total, (PAD, BLOCK))
        peak = jnp.broadcast_to(peak, (PAD, BLOCK))
        block_sum[b] = total
        block_peak[b] = peak
        old_log = running_log[0:PAD]
        merged = jnp.maximum(total + old_log, peak)
        keep = jnp.exp(total + old_log - merged)
        add = jnp.exp(peak - merged)
        running_log[0:PAD] = merged
        running_log[PAD : 2 * PAD] = running_log[PAD : 2 * PAD] + total
        for h in range(heads):
            k = proj[KEY, rows, head_cols(h)].astype(F32)
            wk = (columns[:, PAD + h : PAD + h + 1] * k * key_factor).astype(BF16)
            term = lax.dot_general(
                wk,
                proj[VALUE, rows, head_cols(h)],
                (((0,), (0,)), ((), ())),
                preferred_element_type=F32,
            )
            terms[b, h] = term
            running[h] = keep[h : h + 1] * running[h] + add[h : h + 1] * term

    for h in range(heads):
        seg_memory[h] = running[h].astype(BF16)
    seg_log[...] = running_log[...]

    def seg_copies(target, source, d):
        return [
            pltpu.make_async_remote_copy(
                src_ref=src,
                dst_ref=dst.at[source],
                send_sem=seg_send.at[which, d],
                recv_sem=seg_recv.at[which, source],
                device_id={"sp": target},
                device_id_type=MESH,
            )
            for which, (src, dst) in enumerate(((seg_memory, got_memory), (seg_log, got_log)))
        ]

    for d in range(1, n_sp):

        @pl.when(place + d < n_sp)
        def _(d=d):
            for c in seg_copies(place + d, place, d - 1):
                c.start()

    def finish(slots):
        @pl.loop(slots[0], slots[1])
        def _(slot):
            pltpu.make_async_copy(w_key, weights.at[slot], weight_sem.at[slot]).wait()

            @pl.loop(0, 2)
            def _(index):
                project(slot, rows_of(index, half))

    finish((GATE_IN, CONV_IN + 1))

    @pl.loop(0, nblocks)
    def _(b):
        rows = rows_of(b, BLOCK)
        product = proj[GATE_IN, rows, :].astype(F32) * proj[CONV_IN, rows, :].astype(F32)
        conv_rows[pl.ds(pl.multiple_of(RIM + b * BLOCK, RIM), BLOCK), :] = product.astype(BF16)

    next_place = lax.rem(place + 1, n_sp)
    rim_copy = pltpu.make_async_remote_copy(
        src_ref=conv_rows.at[pl.ds(total_rows, RIM)],
        dst_ref=rim,
        send_sem=rim_sem.at[0],
        recv_sem=rim_sem.at[1],
        device_id={"sp": next_place},
        device_id_type=MESH,
    )

    @pl.when(place + 1 < n_sp)
    def _():
        rim_copy.start()

    finish((GATE_OUT, OUT_GATE + 1))

    @pl.when(place > 0)
    def _():
        rim_copy.wait_recv()
        conv_rows[0:RIM, :] = rim[...]

    @pl.when(place == 0)
    def _():
        conv_rows[0:RIM, :] = jnp.zeros((RIM, width), BF16)

    own_cols = pl.ds(pl.multiple_of(me * width, width), width)
    taps = conv_taps[:, own_cols].astype(F32)
    tap_count = conv_taps.shape[0]

    @pl.loop(0, nblocks)
    def _(b):
        rows = rows_of(b, BLOCK)
        x = conv_rows[pl.ds(pl.multiple_of(b * BLOCK, RIM), BLOCK + RIM), :].astype(F32)
        mixed = None
        for j in range(tap_count):
            back = tap_count - 1 - j
            y = x if back == 0 else pltpu.roll(x, back, 0)
            y = y[RIM:] * taps[j : j + 1]
            mixed = y if mixed is None else mixed + y
        mix[rows, pl.ds(width, width)] = (proj[GATE_OUT, rows, :].astype(F32) * mixed).astype(BF16)

    for h in range(heads):
        running[h] = init_memory[h]
    running_log[0:PAD] = jnp.zeros((PAD, BLOCK), F32)

    def advance(total, peak, term_of):
        old_log = running_log[0:PAD]
        merged = jnp.maximum(total + old_log, peak)
        keep = jnp.exp(total + old_log - merged)
        add = jnp.exp(peak - merged)
        running_log[0:PAD] = merged
        for h in range(heads):
            running[h] = keep[h : h + 1] * running[h] + add[h : h + 1] * term_of(h)

    @pl.loop(0, place)
    def _(source):
        for c in seg_copies(place, source, 0):
            c.wait_recv()
        advance(
            got_log[source, PAD : 2 * PAD],
            got_log[source, 0:PAD],
            lambda h: got_memory[source, h].astype(F32),
        )

    @pl.loop(0, nblocks)
    def _(b):
        starts_log[b] = running_log[0:PAD]
        for h in range(heads):
            starts[b, h] = running[h].astype(BF16)
        advance(block_sum[b], block_peak[b], lambda h: terms[b, h])

    gain = head_gain[:, own_cols].astype(F32)
    causal = col_i <= row_i

    def readout(index):
        @pl.loop(0, half // BLOCK)
        def _(step):
            b = index * (half // BLOCK) + step
            rows = rows_of(b, BLOCK)
            columns = col_log[b]
            for h in range(heads):
                q = proj[QUERY, rows, head_cols(h)]
                k = proj[KEY, rows, head_cols(h)]
                scores = lax.dot_general(
                    q, k, (((1,), (1,)), ((), ())), preferred_element_type=F32
                )
                cum_col = columns[:, h : h + 1]
                pair = (cum_col - row_log[b, h : h + 1]) + row_log[b, PAD + h : PAD + h + 1]
                pair = jnp.where(causal, pair, -jnp.inf)
                carried_log = cum_col + starts_log[b, h : h + 1, 0:1]
                top = jnp.maximum(carried_log, jnp.max(pair, axis=1, keepdims=True))
                weighted = (jnp.exp(pair - top) * (scores * key_factor)).astype(BF16)
                carried = jnp.dot(q, starts[b, h], preferred_element_type=F32)
                out = jnp.exp(carried_log - top) * carried + jnp.dot(
                    weighted, proj[VALUE, rows, head_cols(h)], preferred_element_type=F32
                )
                out = out * lax.rsqrt(jnp.mean(out * out, axis=1, keepdims=True) + EPSILON)
                gate = jax.nn.sigmoid(proj[OUT_GATE, rows, head_cols(h)].astype(F32))
                mix[rows, head_cols(h)] = (out * gain[:, head_cols(h)] * gate).astype(BF16)

    def part_copy(c):
        return pltpu.make_async_remote_copy(
            src_ref=part_send.at[c],
            dst_ref=part_got.at[c],
            send_sem=part_sem_send.at[c],
            recv_sem=part_sem_recv.at[c],
            device_id={"tp": other},
            device_id_type=MESH,
        )

    def partial_rows(index, c):
        return jnp.dot(
            mix[rows_of(index, half), :], out_w[:, rows_of(c, OUT_COLS)], preferred_element_type=F32
        ).astype(BF16)

    readout(other)
    for c in out_copies:
        c.wait()

    @pl.loop(0, n_out)
    def _(c):
        part_send[c] = partial_rows(other, c)
        part_copy(c).start()

    readout(me)

    def result_copy(c):
        return pltpu.make_async_copy(
            result.at[c], layer_out.at[:, rows_of(c, OUT_COLS)], out_sem.at[c]
        )

    @pl.loop(0, n_out)
    def _(c):
        own = partial_rows(me, c)
        part_copy(c).wait_recv()
        result[c] = (own.astype(F32) + part_got[c].astype(F32)).astype(BF16)
        result_copy(c).start()

    token_copy.wait_send()

    @pl.when(place + 1 < n_sp)
    def _():
        rim_copy.wait_send()

    for d in range(1, n_sp):

        @pl.when(place + d < n_sp)
        def _(d=d):
            for c in seg_copies(place + d, place, d - 1):
                c.wait_send()

    @pl.loop(0, n_out)
    def _(c):
        part_copy(c).wait_send()
        result_copy(c).wait()


def local(
    tokens,
    norm_gain,
    w_query,
    w_key,
    w_value,
    w_outgate,
    w_gatein,
    w_gateout,
    w_convin,
    w_igate,
    w_fgate,
    input_bias,
    forget_bias,
    forget_extra,
    init_memory,
    head_gain,
    conv_taps,
    out_memory,
    out_conv,
):
    heads, dh = init_memory.shape[1], init_memory.shape[2]
    half, features = tokens.shape[1], tokens.shape[2]
    rows = forget_extra.shape[1]
    width = w_query.shape[1]
    nblocks = rows // BLOCK
    n_sp = lax.axis_size("sp")
    first = lax.axis_index("tp") * heads

    def own(a, axis):
        return lax.dynamic_slice_in_dim(a, first, heads, axis)

    gate_w = jnp.concatenate(
        [
            own(w_fgate, 1),
            jnp.zeros((features, PAD - heads), BF16),
            own(w_igate, 1),
            jnp.zeros((features, BLOCK - PAD - heads), BF16),
        ],
        axis=1,
    )
    gap = jnp.zeros((PAD - heads,), F32)
    gate_bias = jnp.concatenate([own(forget_bias, 0), gap, own(input_bias, 0), gap])
    gate_bias = jnp.broadcast_to(gate_bias[:, None], (2 * PAD, BLOCK))
    extra = jnp.pad(jnp.transpose(forget_extra[0]), ((0, PAD - heads), (0, 0)))

    vmem = pl.BlockSpec(memory_space=pltpu.VMEM)
    hbm = pl.BlockSpec(memory_space=pl.ANY)
    dma = pltpu.SemaphoreType.DMA
    n_seg = max(n_sp - 1, 1)
    n_out = features // OUT_COLS
    out = pl.pallas_call(
        functools.partial(kernel, n_sp),
        name="layer",
        out_shape=jax.ShapeDtypeStruct((half, features), BF16),
        in_specs=[hbm, vmem] + [hbm] * 7 + [vmem] * 6 + [hbm] * 2,
        out_specs=hbm,
        scratch_shapes=[
            pltpu.VMEM((2, half, features), BF16),
            pltpu.VMEM((rows, features), BF16),
            pltpu.VMEM((7, features, width), BF16),
            pltpu.VMEM((2 * width, features), BF16),
            pltpu.VMEM((7, rows, width), BF16),
            pltpu.VMEM((rows, BLOCK), F32),
            pltpu.VMEM((nblocks, 2 * PAD, BLOCK), F32),
            pltpu.VMEM((nblocks, BLOCK, BLOCK), F32),
            pltpu.VMEM((nblocks, PAD, BLOCK), F32),
            pltpu.VMEM((nblocks, PAD, BLOCK), F32),
            pltpu.VMEM((nblocks, heads, dh, dh), F32),
            pltpu.VMEM((heads, dh, dh), F32),
            pltpu.VMEM((2 * PAD, BLOCK), F32),
            pltpu.VMEM((nblocks, heads, dh, dh), BF16),
            pltpu.VMEM((nblocks, PAD, BLOCK), F32),
            pltpu.VMEM((heads, dh, dh), BF16),
            pltpu.VMEM((2 * PAD, BLOCK), F32),
            pltpu.VMEM((n_seg, heads, dh, dh), BF16),
            pltpu.VMEM((n_seg, 2 * PAD, BLOCK), F32),
            pltpu.VMEM((RIM + rows, width), BF16),
            pltpu.VMEM((RIM, width), BF16),
            pltpu.VMEM((rows, 2 * width), BF16),
            pltpu.VMEM((n_out, half, OUT_COLS), BF16),
            pltpu.VMEM((n_out, half, OUT_COLS), BF16),
            pltpu.VMEM((n_out, half, OUT_COLS), BF16),
            dma((1,)),
            dma((9,)),
            dma((n_out,)),
            dma((2,)),
            dma((2, n_seg)),
            dma((2, n_seg)),
            dma((2,)),
            dma((n_out,)),
            dma((n_out,)),
        ],
        compiler_params=pltpu.CompilerParams(
            collective_id=0, has_side_effects=True, vmem_limit_bytes=63 * 1024 * 1024
        ),
    )(
        tokens[0],
        norm_gain.reshape(1, features),
        w_key,
        w_value,
        w_gatein,
        w_convin,
        w_gateout,
        w_query,
        w_outgate,
        gate_w,
        gate_bias,
        extra,
        init_memory[0],
        head_gain.reshape(1, -1),
        conv_taps,
        out_memory,
        out_conv,
    )
    return out[None]


def solution(mesh):
    return jax.shard_map(
        local,
        mesh=mesh,
        in_specs=(
            P("fs", ("sp", "tp"), None),
            P(),
            P(None, "tp"),
            P(None, "tp"),
            P(None, "tp"),
            P(None, "tp"),
            P(None, "tp"),
            P(None, "tp"),
            P(None, "tp"),
            P(),
            P(),
            P(),
            P(),
            P("fs", "sp", "tp"),
            P("fs", "tp", None, None),
            P(),
            P(),
            P("tp", None),
            P("tp", None),
        ),
        out_specs=P("fs", ("sp", "tp"), None),
        check_vma=False,
    )
```

```python
import functools

import jax
import jax.numpy as jnp
from jax import lax
from jax.experimental import pallas as pl
from jax.experimental.pallas import tpu as pltpu
from jax.sharding import PartitionSpec as P

BLOCK = 128
EPSILON = 1e-06
LOWEST_LOG = -1e30
MESH = pl.DeviceIdType.MESH
F32 = jnp.float32
BF16 = jnp.bfloat16
PAD = 8
RIM = 16
NORM_ROWS = 64

KEY, VALUE, GATE_IN, CONV_IN, GATE_OUT, QUERY, OUT_GATE = range(7)


def kernel(
    n_sp,
    tokens,
    norm_gain,
    w_key,
    w_value,
    w_gatein,
    w_convin,
    w_gateout,
    w_query,
    w_outgate,
    w_igate,
    w_fgate,
    input_bias,
    forget_bias,
    extra,
    init_memory,
    head_gain,
    conv_taps,
    out_memory,
    out_conv,
    layer_out,
    tok,
    gain_row,
    head_rows,
    gate_w,
    normed,
    weights,
    out_w,
    proj,
    gate_pre,
    row_log,
    col_log,
    block_sum,
    block_peak,
    terms,
    running,
    running_log,
    starts,
    starts_log,
    seg_memory,
    seg_log,
    got_memory,
    got_log,
    conv_rows,
    rim,
    mix,
    part_send,
    part_got,
    local_sem,
    weight_sem,
    token_sem,
    seg_send,
    seg_recv,
    rim_sem,
    part_sem_send,
    part_sem_recv,
):
    me = lax.axis_index("tp")
    other = 1 - me
    place = lax.axis_index("sp")
    half = tok.shape[1]
    total_rows = normed.shape[0]
    width = w_key.shape[1]
    heads = init_memory.shape[0]
    dh = init_memory.shape[1]
    nblocks = total_rows // BLOCK
    key_factor = dh ** (-0.5)
    out_width = layer_out.shape[1]
    n_out = half // BLOCK
    out_cols = out_width // n_out

    barrier = pltpu.get_barrier_semaphore()
    pl.semaphore_signal(barrier, inc=1, device_id={"tp": other}, device_id_type=MESH)
    for d in range(1, n_sp):
        pl.semaphore_signal(
            barrier, inc=1, device_id={"sp": lax.rem(place + d, n_sp)}, device_id_type=MESH
        )

    own_copy = pltpu.make_async_copy(tokens, tok.at[0], local_sem.at[0])
    own_copy.start()
    w_in = (w_key, w_value, w_gatein, w_convin, w_gateout, w_query, w_outgate)
    w_copies = [
        pltpu.make_async_copy(w, weights.at[s], weight_sem.at[s]) for s, w in enumerate(w_in)
    ]
    out_copies = [
        pltpu.make_async_copy(out_memory, out_w.at[pl.ds(0, width)], weight_sem.at[7]),
        pltpu.make_async_copy(out_conv, out_w.at[pl.ds(width, width)], weight_sem.at[8]),
    ]
    for c in w_copies + out_copies:
        c.start()

    pl.semaphore_wait(barrier, n_sp)
    token_copy = pltpu.make_async_remote_copy(
        src_ref=tokens,
        dst_ref=tok.at[1],
        send_sem=token_sem.at[0],
        recv_sem=token_sem.at[1],
        device_id={"tp": other},
        device_id_type=MESH,
    )
    token_copy.start()

    gates = jnp.concatenate(
        [w_fgate[...], w_igate[...], jnp.zeros((BLOCK - 2 * PAD, w_igate.shape[1]), BF16)], axis=0
    )
    gate_w[...] = jnp.transpose(gates)
    for j in range(norm_gain.shape[0]):
        gain_row[:, j * BLOCK : (j + 1) * BLOCK] = norm_gain[j : j + 1].astype(F32)
    head_rows[...] = head_gain[...].astype(F32)
    own_copy.wait()

    def rows_of(index, size):
        return pl.ds(pl.multiple_of(index * size, size), size)

    def normalize(slot, base):
        @pl.loop(0, half // NORM_ROWS)
        def _(c):
            x = tok[slot, rows_of(c, NORM_ROWS), :].astype(F32)
            scale = lax.rsqrt(jnp.mean(x * x, axis=-1, keepdims=True) + EPSILON)
            y = (x * scale) * gain_row[...]
            normed[pl.ds(pl.multiple_of(base + c * NORM_ROWS, NORM_ROWS), NORM_ROWS), :] = y.astype(
                BF16
            )

    def project(slot, rows):
        proj[slot, rows, :] = jnp.dot(
            normed[rows, :], weights[slot], preferred_element_type=F32
        ).astype(BF16)

    @pl.loop(0, 2)
    def _(step):
        index = lax.rem(me + step, 2)

        @pl.when(step == 1)
        def _():
            token_copy.wait_recv()

        normalize(step, index * half)
        rows = rows_of(index, half)
        gate_pre[rows, :] = jnp.dot(normed[rows, :], gate_w[...], preferred_element_type=F32)

        @pl.loop(KEY, VALUE + 1)
        def _(slot):
            @pl.when(step == 0)
            def _():
                pltpu.make_async_copy(w_key, weights.at[slot], weight_sem.at[slot]).wait()

            project(slot, rows)

    row_i = lax.broadcasted_iota(jnp.int32, (BLOCK, BLOCK), 0)
    col_i = lax.broadcasted_iota(jnp.int32, (BLOCK, BLOCK), 1)
    upper = jnp.where(row_i <= col_i, 1.0, 0.0).astype(F32)
    for h in range(heads):
        running[h] = jnp.zeros((dh, dh), F32)
    running_log[0:PAD] = jnp.full((PAD, BLOCK), LOWEST_LOG, F32)
    running_log[PAD : 2 * PAD] = jnp.zeros((PAD, BLOCK), F32)

    def head_cols(h):
        return slice(h * dh, (h + 1) * dh)

    first_head = me * heads
    to_front = lax.rem(PAD - first_head, PAD)
    lane_head = lax.broadcasted_iota(jnp.int32, (PAD, BLOCK), 0)
    bias_f = jnp.zeros((PAD, BLOCK), F32)
    bias_i = jnp.zeros((PAD, BLOCK), F32)
    for h in range(heads):
        bias_f = jnp.where(lane_head == h, forget_bias[first_head + h], bias_f)
        bias_i = jnp.where(lane_head == h, input_bias[first_head + h], bias_i)
    no_head = jnp.zeros((PAD - heads, BLOCK), F32)

    forget_rows, in_rows = [], []
    for b in range(nblocks):
        span = slice(b * BLOCK, (b + 1) * BLOCK)
        pre = jnp.transpose(gate_pre[span, :])
        v = pltpu.roll(pre[0:PAD], to_front, 0) + bias_f
        log_forget = jnp.minimum(v, 0.0) - jnp.log1p(jnp.exp(-jnp.abs(v)))
        forget_rows.append(log_forget + jnp.concatenate([extra[:, span], no_head], axis=0))
        in_rows.append(pltpu.roll(pre[PAD : 2 * PAD], to_front, 0) + bias_i)
    all_cumulative = jnp.dot(
        jnp.concatenate(forget_rows, axis=0),
        upper,
        precision=lax.Precision.HIGHEST,
        preferred_element_type=F32,
    )
    all_in = jnp.concatenate(in_rows, axis=0)
    all_total = jnp.broadcast_to(all_cumulative[:, BLOCK - 1 : BLOCK], all_in.shape)
    exponent = all_total - all_cumulative + all_in
    all_peak = jnp.broadcast_to(jnp.max(exponent, axis=1, keepdims=True), all_in.shape)
    key_weight = jnp.exp(exponent - all_peak)
    filler = jnp.zeros((BLOCK - 2 * PAD, BLOCK), F32)
    for b in range(nblocks):
        span = slice(b * PAD, (b + 1) * PAD)
        row_log[b, 0:PAD] = all_cumulative[span]
        row_log[b, PAD : 2 * PAD] = all_in[span]
        block_sum[b] = all_total[span]
        block_peak[b] = all_peak[span]
        col_log[b] = jnp.transpose(
            jnp.concatenate([all_cumulative[span], key_weight[span], filler], axis=0)
        )

    @pl.loop(0, nblocks, unroll=2)
    def _(b):
        rows = rows_of(b, BLOCK)
        columns = col_log[b]
        total, peak = block_sum[b], block_peak[b]
        old_log = running_log[0:PAD]
        merged = jnp.maximum(total + old_log, peak)
        keep = jnp.exp(total + old_log - merged)
        add = jnp.exp(peak - merged)
        running_log[0:PAD] = merged
        running_log[PAD : 2 * PAD] = running_log[PAD : 2 * PAD] + total
        for h in range(heads):
            k = proj[KEY, rows, head_cols(h)].astype(F32)
            wk = (columns[:, PAD + h : PAD + h + 1] * k * key_factor).astype(BF16)
            term = lax.dot_general(
                wk,
                proj[VALUE, rows, head_cols(h)],
                (((0,), (0,)), ((), ())),
                preferred_element_type=F32,
            )
            terms[b, h] = term
            running[h] = keep[h : h + 1] * running[h] + add[h : h + 1] * term

    for h in range(heads):
        seg_memory[h] = running[h].astype(BF16)
    seg_log[...] = running_log[...]

    def seg_copies(target, source, d):
        return [
            pltpu.make_async_remote_copy(
                src_ref=src,
                dst_ref=dst.at[source],
                send_sem=seg_send.at[which, d],
                recv_sem=seg_recv.at[which, source],
                device_id={"sp": target},
                device_id_type=MESH,
            )
            for which, (src, dst) in enumerate(((seg_memory, got_memory), (seg_log, got_log)))
        ]

    for d in range(1, n_sp):

        @pl.when(place + d < n_sp)
        def _(d=d):
            for c in seg_copies(place + d, place, d - 1):
                c.start()

    def finish(slots):
        @pl.loop(slots[0], slots[1])
        def _(slot):
            pltpu.make_async_copy(w_key, weights.at[slot], weight_sem.at[slot]).wait()

            @pl.loop(0, 2)
            def _(index):
                project(slot, rows_of(index, half))

    finish((GATE_IN, CONV_IN + 1))

    @pl.loop(0, nblocks)
    def _(b):
        rows = rows_of(b, BLOCK)
        product = proj[GATE_IN, rows, :].astype(F32) * proj[CONV_IN, rows, :].astype(F32)
        conv_rows[pl.ds(pl.multiple_of(RIM + b * BLOCK, RIM), BLOCK), :] = product.astype(BF16)

    next_place = lax.rem(place + 1, n_sp)
    rim_copy = pltpu.make_async_remote_copy(
        src_ref=conv_rows.at[pl.ds(total_rows, RIM)],
        dst_ref=rim,
        send_sem=rim_sem.at[0],
        recv_sem=rim_sem.at[1],
        device_id={"sp": next_place},
        device_id_type=MESH,
    )

    @pl.when(place + 1 < n_sp)
    def _():
        rim_copy.start()

    finish((GATE_OUT, OUT_GATE + 1))

    @pl.when(place > 0)
    def _():
        rim_copy.wait_recv()
        conv_rows[0:RIM, :] = rim[...]

    @pl.when(place == 0)
    def _():
        conv_rows[0:RIM, :] = jnp.zeros((RIM, width), BF16)

    own_cols = pl.ds(pl.multiple_of(me * width, width), width)
    taps = conv_taps[:, own_cols].astype(F32)
    tap_count = conv_taps.shape[0]

    @pl.loop(0, nblocks)
    def _(b):
        rows = rows_of(b, BLOCK)
        x = conv_rows[pl.ds(pl.multiple_of(b * BLOCK, RIM), BLOCK + RIM), :].astype(F32)
        mixed = None
        for j in range(tap_count):
            back = tap_count - 1 - j
            y = x if back == 0 else pltpu.roll(x, back, 0)
            y = y[RIM:] * taps[j : j + 1]
            mixed = y if mixed is None else mixed + y
        mix[rows, pl.ds(width, width)] = (proj[GATE_OUT, rows, :].astype(F32) * mixed).astype(BF16)

    for h in range(heads):
        running[h] = init_memory[h]
    running_log[0:PAD] = jnp.zeros((PAD, BLOCK), F32)

    def advance(total, peak, term_of):
        old_log = running_log[0:PAD]
        merged = jnp.maximum(total + old_log, peak)
        keep = jnp.exp(total + old_log - merged)
        add = jnp.exp(peak - merged)
        running_log[0:PAD] = merged
        for h in range(heads):
            running[h] = keep[h : h + 1] * running[h] + add[h : h + 1] * term_of(h)

    @pl.loop(0, place)
    def _(source):
        for c in seg_copies(place, source, 0):
            c.wait_recv()
        advance(
            got_log[source, PAD : 2 * PAD],
            got_log[source, 0:PAD],
            lambda h: got_memory[source, h].astype(F32),
        )

    @pl.loop(0, nblocks)
    def _(b):
        starts_log[b] = running_log[0:PAD]
        for h in range(heads):
            starts[b, h] = running[h].astype(BF16)
        advance(block_sum[b], block_peak[b], lambda h: terms[b, h])

    causal = col_i <= row_i

    def read_block(b):
        rows = rows_of(b, BLOCK)
        columns = col_log[b]
        for h in range(heads):
            q = proj[QUERY, rows, head_cols(h)]
            k = proj[KEY, rows, head_cols(h)]
            scores = lax.dot_general(
                q, k, (((1,), (1,)), ((), ())), preferred_element_type=F32
            )
            cum_col = columns[:, h : h + 1]
            pair = (cum_col - row_log[b, h : h + 1]) + row_log[b, PAD + h : PAD + h + 1]
            pair = jnp.where(causal, pair, -jnp.inf)
            carried_log = cum_col + starts_log[b, h : h + 1, 0:1]
            top = jnp.maximum(carried_log, jnp.max(pair, axis=1, keepdims=True))
            weighted = (jnp.exp(pair - top) * (scores * key_factor)).astype(BF16)
            carried = jnp.dot(q, starts[b, h], preferred_element_type=F32)
            out = jnp.exp(carried_log - top) * carried + jnp.dot(
                weighted, proj[VALUE, rows, head_cols(h)], preferred_element_type=F32
            )
            out = out * lax.rsqrt(jnp.mean(out * out, axis=1, keepdims=True) + EPSILON)
            gate = jax.nn.sigmoid(proj[OUT_GATE, rows, head_cols(h)].astype(F32))
            mix[rows, head_cols(h)] = (out * head_rows[pl.ds(first_head + h, 1), :] * gate).astype(BF16)

    def part_copy(c):
        return pltpu.make_async_remote_copy(
            src_ref=part_send.at[c],
            dst_ref=part_got.at[c],
            send_sem=part_sem_send.at[c],
            recv_sem=part_sem_recv.at[c],
            device_id={"tp": other},
            device_id_type=MESH,
        )

    def partial_rows(index, c):
        return jnp.dot(
            mix[rows_of(index, half), :], out_w[:, rows_of(c, out_cols)], preferred_element_type=F32
        ).astype(BF16)

    @pl.loop(0, n_out)
    def _(step):
        read_block(other * n_out + step)

    for c in out_copies:
        c.wait()

    @pl.loop(0, n_out)
    def _(step):
        part_send[step] = partial_rows(other, step)
        read_block(me * n_out + step)
        part_copy(step).start()

    @pl.loop(0, n_out)
    def _(c):
        own = partial_rows(me, c)
        part_copy(c).wait_recv()
        total = own.astype(F32) + part_got[c].astype(F32)
        layer_out[:, rows_of(c, out_cols)] = total.astype(BF16)

    token_copy.wait_send()

    @pl.when(place + 1 < n_sp)
    def _():
        rim_copy.wait_send()

    for d in range(1, n_sp):

        @pl.when(place + d < n_sp)
        def _(d=d):
            for c in seg_copies(place + d, place, d - 1):
                c.wait_send()

    @pl.loop(0, n_out)
    def _(c):
        part_copy(c).wait_send()


def local(
    tokens,
    norm_gain,
    w_query,
    w_key,
    w_value,
    w_outgate,
    w_gatein,
    w_gateout,
    w_convin,
    w_igate,
    w_fgate,
    input_bias,
    forget_bias,
    forget_extra,
    init_memory,
    head_gain,
    conv_taps,
    out_memory,
    out_conv,
):
    heads, dh = init_memory.shape[1], init_memory.shape[2]
    half, features = tokens.shape[1], tokens.shape[2]
    rows = forget_extra.shape[1]
    width = w_query.shape[1]
    nblocks = rows // BLOCK
    n_sp = lax.axis_size("sp")
    vmem = pl.BlockSpec(memory_space=pltpu.VMEM)
    hbm = pl.BlockSpec(memory_space=pl.ANY)
    smem = pl.BlockSpec(memory_space=pltpu.SMEM)
    dma = pltpu.SemaphoreType.DMA
    n_seg = max(n_sp - 1, 1)
    n_out = half // BLOCK
    out_cols = features // n_out
    out = pl.pallas_call(
        functools.partial(kernel, n_sp),
        name="layer",
        out_shape=pltpu.VMEM((half, features), BF16),
        in_specs=[hbm, vmem] + [hbm] * 7 + [vmem] * 2 + [smem] * 2 + [vmem] * 4 + [hbm] * 2,
        out_specs=vmem,
        scratch_shapes=[
            pltpu.VMEM((2, half, features), BF16),
            pltpu.VMEM((1, features), F32),
            pltpu.VMEM((PAD, BLOCK), F32),
            pltpu.VMEM((features, BLOCK), BF16),
            pltpu.VMEM((rows, features), BF16),
            pltpu.VMEM((7, features, width), BF16),
            pltpu.VMEM((2 * width, features), BF16),
            pltpu.VMEM((7, rows, width), BF16),
            pltpu.VMEM((rows, BLOCK), F32),
            pltpu.VMEM((nblocks, 2 * PAD, BLOCK), F32),
            pltpu.VMEM((nblocks, BLOCK, BLOCK), F32),
            pltpu.VMEM((nblocks, PAD, BLOCK), F32),
            pltpu.VMEM((nblocks, PAD, BLOCK), F32),
            pltpu.VMEM((nblocks, heads, dh, dh), F32),
            pltpu.VMEM((heads, dh, dh), F32),
            pltpu.VMEM((2 * PAD, BLOCK), F32),
            pltpu.VMEM((nblocks, heads, dh, dh), BF16),
            pltpu.VMEM((nblocks, PAD, BLOCK), F32),
            pltpu.VMEM((heads, dh, dh), BF16),
            pltpu.VMEM((2 * PAD, BLOCK), F32),
            pltpu.VMEM((n_seg, heads, dh, dh), BF16),
            pltpu.VMEM((n_seg, 2 * PAD, BLOCK), F32),
            pltpu.VMEM((RIM + rows, width), BF16),
            pltpu.VMEM((RIM, width), BF16),
            pltpu.VMEM((rows, 2 * width), BF16),
            pltpu.VMEM((n_out, half, out_cols), BF16),
            pltpu.VMEM((n_out, half, out_cols), BF16),
            dma((1,)),
            dma((9,)),
            dma((2,)),
            dma((2, n_seg)),
            dma((2, n_seg)),
            dma((2,)),
            dma((n_out,)),
            dma((n_out,)),
        ],
        compiler_params=pltpu.CompilerParams(
            collective_id=0, has_side_effects=True, vmem_limit_bytes=60 * 1024 * 1024
        ),
    )(
        tokens[0],
        norm_gain.reshape(-1, BLOCK),
        w_key,
        w_value,
        w_gatein,
        w_convin,
        w_gateout,
        w_query,
        w_outgate,
        jnp.transpose(w_igate),
        jnp.transpose(w_fgate),
        input_bias,
        forget_bias,
        jnp.transpose(forget_extra[0]),
        init_memory[0],
        head_gain.reshape(-1, dh),
        conv_taps,
        out_memory,
        out_conv,
    )
    return out[None]


def solution(mesh):
    return jax.shard_map(
        local,
        mesh=mesh,
        in_specs=(
            P("fs", ("sp", "tp"), None),
            P(),
            P(None, "tp"),
            P(None, "tp"),
            P(None, "tp"),
            P(None, "tp"),
            P(None, "tp"),
            P(None, "tp"),
            P(None, "tp"),
            P(),
            P(),
            P(),
            P(),
            P("fs", "sp", "tp"),
            P("fs", "tp", None, None),
            P(),
            P(),
            P("tp", None),
            P("tp", None),
        ),
        out_specs=P("fs", ("sp", "tp"), None),
        check_vma=False,
    )
```

```python
import functools

import jax
import jax.numpy as jnp
from jax import lax
from jax.experimental import pallas as pl
from jax.experimental.pallas import tpu as pltpu
from jax.sharding import PartitionSpec as P

BLOCK = 128
EPSILON = 1e-06
LOWEST_LOG = -1e30
MESH = pl.DeviceIdType.MESH
F32 = jnp.float32
BF16 = jnp.bfloat16
PAD = 8
RIM = 16
NORM_ROWS = 64

KEY, VALUE, QUERY, GATE_IN, CONV_IN, GATE_OUT, OUT_GATE = range(7)


def kernel(
    n_sp,
    tokens,
    norm_gain,
    w_key,
    w_value,
    w_gatein,
    w_convin,
    w_gateout,
    w_query,
    w_outgate,
    w_igate,
    w_fgate,
    input_bias,
    forget_bias,
    extra,
    init_memory,
    head_gain,
    conv_taps,
    out_memory,
    out_conv,
    layer_out,
    tok,
    gain_row,
    head_rows,
    gate_w,
    normed,
    weights,
    out_w,
    proj,
    gate_pre,
    row_log,
    col_log,
    block_sum,
    block_peak,
    terms,
    within,
    peak_log,
    running,
    running_log,
    starts,
    starts_log,
    seg_memory,
    seg_log,
    got_memory,
    got_log,
    conv_rows,
    rim,
    mix,
    part_send,
    part_got,
    local_sem,
    weight_sem,
    token_sem,
    seg_send,
    seg_recv,
    rim_sem,
    part_sem_send,
    part_sem_recv,
):
    me = lax.axis_index("tp")
    other = 1 - me
    place = lax.axis_index("sp")
    half = tok.shape[1]
    total_rows = normed.shape[0]
    width = w_key.shape[1]
    heads = init_memory.shape[0]
    dh = init_memory.shape[1]
    nblocks = total_rows // BLOCK
    key_factor = dh ** (-0.5)
    out_width = layer_out.shape[1]
    n_out = half // BLOCK
    out_cols = out_width // n_out

    barrier = pltpu.get_barrier_semaphore()
    pl.semaphore_signal(barrier, inc=1, device_id={"tp": other}, device_id_type=MESH)
    for d in range(1, n_sp):
        pl.semaphore_signal(
            barrier, inc=1, device_id={"sp": lax.rem(place + d, n_sp)}, device_id_type=MESH
        )

    own_copy = pltpu.make_async_copy(tokens, tok.at[0], local_sem.at[0])
    own_copy.start()
    w_in = (w_key, w_value, w_query, w_gatein, w_convin, w_gateout, w_outgate)
    w_copies = [
        pltpu.make_async_copy(w, weights.at[s], weight_sem.at[s]) for s, w in enumerate(w_in)
    ]
    out_copies = [
        pltpu.make_async_copy(out_memory, out_w.at[pl.ds(0, width)], weight_sem.at[7]),
        pltpu.make_async_copy(out_conv, out_w.at[pl.ds(width, width)], weight_sem.at[8]),
    ]
    for c in w_copies[:2]:
        c.start()

    pl.semaphore_wait(barrier, n_sp)
    token_copy = pltpu.make_async_remote_copy(
        src_ref=tokens,
        dst_ref=tok.at[1],
        send_sem=token_sem.at[0],
        recv_sem=token_sem.at[1],
        device_id={"tp": other},
        device_id_type=MESH,
    )
    token_copy.start()

    gates = jnp.concatenate(
        [w_fgate[...], w_igate[...], jnp.zeros((BLOCK - 2 * PAD, w_igate.shape[1]), BF16)], axis=0
    )
    gate_w[...] = jnp.transpose(gates)
    for j in range(norm_gain.shape[0]):
        gain_row[:, j * BLOCK : (j + 1) * BLOCK] = norm_gain[j : j + 1].astype(F32)
    head_rows[...] = head_gain[...].astype(F32)
    own_copy.wait()
    for c in w_copies[2:] + out_copies:
        c.start()

    def rows_of(index, size):
        return pl.ds(pl.multiple_of(index * size, size), size)

    def normalize(slot, base):
        @pl.loop(0, half // NORM_ROWS)
        def _(c):
            x = tok[slot, rows_of(c, NORM_ROWS), :].astype(F32)
            scale = lax.rsqrt(jnp.mean(x * x, axis=-1, keepdims=True) + EPSILON)
            y = (x * scale) * gain_row[...]
            normed[pl.ds(pl.multiple_of(base + c * NORM_ROWS, NORM_ROWS), NORM_ROWS), :] = y.astype(
                BF16
            )

    def project(slot, rows):
        proj[slot, rows, :] = jnp.dot(
            normed[rows, :], weights[slot], preferred_element_type=F32
        ).astype(BF16)

    @pl.loop(0, 2)
    def _(step):
        index = lax.rem(me + step, 2)

        @pl.when(step == 1)
        def _():
            token_copy.wait_recv()

        normalize(step, index * half)
        rows = rows_of(index, half)
        gate_pre[rows, :] = jnp.dot(normed[rows, :], gate_w[...], preferred_element_type=F32)

        @pl.loop(KEY, VALUE + 1)
        def _(slot):
            @pl.when(step == 0)
            def _():
                pltpu.make_async_copy(w_key, weights.at[slot], weight_sem.at[slot]).wait()

            project(slot, rows)

    row_i = lax.broadcasted_iota(jnp.int32, (BLOCK, BLOCK), 0)
    col_i = lax.broadcasted_iota(jnp.int32, (BLOCK, BLOCK), 1)
    upper = jnp.where(row_i <= col_i, 1.0, 0.0).astype(F32)
    for h in range(heads):
        running[h] = jnp.zeros((dh, dh), F32)
    running_log[0:PAD] = jnp.full((PAD, BLOCK), LOWEST_LOG, F32)
    running_log[PAD : 2 * PAD] = jnp.zeros((PAD, BLOCK), F32)

    def head_cols(h):
        return slice(h * dh, (h + 1) * dh)

    first_head = me * heads
    to_front = lax.rem(PAD - first_head, PAD)
    lane_head = lax.broadcasted_iota(jnp.int32, (PAD, BLOCK), 0)
    bias_f = jnp.zeros((PAD, BLOCK), F32)
    bias_i = jnp.zeros((PAD, BLOCK), F32)
    for h in range(heads):
        bias_f = jnp.where(lane_head == h, forget_bias[first_head + h], bias_f)
        bias_i = jnp.where(lane_head == h, input_bias[first_head + h], bias_i)
    no_head = jnp.zeros((PAD - heads, BLOCK), F32)

    forget_rows, in_rows = [], []
    for b in range(nblocks):
        span = slice(b * BLOCK, (b + 1) * BLOCK)
        pre = jnp.transpose(gate_pre[span, :])
        v = pltpu.roll(pre[0:PAD], to_front, 0) + bias_f
        log_forget = jnp.minimum(v, 0.0) - jnp.log1p(jnp.exp(-jnp.abs(v)))
        forget_rows.append(log_forget + jnp.concatenate([extra[:, span], no_head], axis=0))
        in_rows.append(pltpu.roll(pre[PAD : 2 * PAD], to_front, 0) + bias_i)
    all_cumulative = jnp.dot(
        jnp.concatenate(forget_rows, axis=0),
        upper,
        precision=lax.Precision.HIGHEST,
        preferred_element_type=F32,
    )
    all_in = jnp.concatenate(in_rows, axis=0)
    all_total = jnp.broadcast_to(all_cumulative[:, BLOCK - 1 : BLOCK], all_in.shape)
    exponent = all_total - all_cumulative + all_in
    all_peak = jnp.broadcast_to(jnp.max(exponent, axis=1, keepdims=True), all_in.shape)
    key_weight = jnp.exp(exponent - all_peak)
    filler = jnp.zeros((BLOCK - 2 * PAD, BLOCK), F32)
    for b in range(nblocks):
        span = slice(b * PAD, (b + 1) * PAD)
        row_log[b, 0:PAD] = all_cumulative[span]
        row_log[b, PAD : 2 * PAD] = all_in[span]
        block_sum[b] = all_total[span]
        block_peak[b] = all_peak[span]
        col_log[b] = jnp.transpose(
            jnp.concatenate([all_cumulative[span], key_weight[span], filler], axis=0)
        )

    @pl.loop(0, nblocks, unroll=2)
    def _(b):
        rows = rows_of(b, BLOCK)
        columns = col_log[b]
        total, peak = block_sum[b], block_peak[b]
        old_log = running_log[0:PAD]
        merged = jnp.maximum(total + old_log, peak)
        keep = jnp.exp(total + old_log - merged)
        add = jnp.exp(peak - merged)
        running_log[0:PAD] = merged
        running_log[PAD : 2 * PAD] = running_log[PAD : 2 * PAD] + total
        for h in range(heads):
            k = proj[KEY, rows, head_cols(h)].astype(F32)
            wk = (columns[:, PAD + h : PAD + h + 1] * k * key_factor).astype(BF16)
            term = lax.dot_general(
                wk,
                proj[VALUE, rows, head_cols(h)],
                (((0,), (0,)), ((), ())),
                preferred_element_type=F32,
            )
            terms[b, h] = term
            running[h] = keep[h : h + 1] * running[h] + add[h : h + 1] * term

    for h in range(heads):
        seg_memory[h] = running[h].astype(BF16)
    seg_log[...] = running_log[...]

    def seg_copies(target, source, d):
        return [
            pltpu.make_async_remote_copy(
                src_ref=src,
                dst_ref=dst.at[source],
                send_sem=seg_send.at[which, d],
                recv_sem=seg_recv.at[which, source],
                device_id={"sp": target},
                device_id_type=MESH,
            )
            for which, (src, dst) in enumerate(((seg_memory, got_memory), (seg_log, got_log)))
        ]

    for d in range(1, n_sp):

        @pl.when(place + d < n_sp)
        def _(d=d):
            for c in seg_copies(place + d, place, d - 1):
                c.start()

    causal = col_i <= row_i

    def own_terms(b):
        rows = rows_of(b, BLOCK)
        columns = col_log[b]
        for h in range(heads):
            q = proj[QUERY, rows, head_cols(h)]
            k = proj[KEY, rows, head_cols(h)]
            scores = lax.dot_general(q, k, (((1,), (1,)), ((), ())), preferred_element_type=F32)
            pair = (columns[:, h : h + 1] - row_log[b, h : h + 1]) + row_log[
                b, PAD + h : PAD + h + 1
            ]
            pair = jnp.where(causal, pair, -jnp.inf)
            peak = jnp.max(pair, axis=1, keepdims=True)
            weighted = (jnp.exp(pair - peak) * (scores * key_factor)).astype(BF16)
            peak_log[b, :, h : h + 1] = peak
            within[b, h] = jnp.dot(
                weighted, proj[VALUE, rows, head_cols(h)], preferred_element_type=F32
            )

    def weight_wait(slot):
        pltpu.make_async_copy(w_key, weights.at[slot], weight_sem.at[slot]).wait()

    weight_wait(QUERY)

    @pl.loop(0, 2)
    def _(index):
        project(QUERY, rows_of(index, half))

    per_job = nblocks // 8

    def finish(slots):
        @pl.loop(2 * slots[0], 2 * slots[1])
        def _(job):
            slot = job // 2
            index = lax.rem(job, 2)

            @pl.when(index == 0)
            def _():
                weight_wait(slot)

            project(slot, rows_of(index, half))
            for i in range(per_job):
                own_terms((job - 2 * GATE_IN) * per_job + i)

    finish((GATE_IN, CONV_IN + 1))

    @pl.loop(0, nblocks)
    def _(b):
        rows = rows_of(b, BLOCK)
        product = proj[GATE_IN, rows, :].astype(F32) * proj[CONV_IN, rows, :].astype(F32)
        conv_rows[pl.ds(pl.multiple_of(RIM + b * BLOCK, RIM), BLOCK), :] = product.astype(BF16)

    next_place = lax.rem(place + 1, n_sp)
    rim_copy = pltpu.make_async_remote_copy(
        src_ref=conv_rows.at[pl.ds(total_rows, RIM)],
        dst_ref=rim,
        send_sem=rim_sem.at[0],
        recv_sem=rim_sem.at[1],
        device_id={"sp": next_place},
        device_id_type=MESH,
    )

    @pl.when(place + 1 < n_sp)
    def _():
        rim_copy.start()

    finish((GATE_OUT, OUT_GATE + 1))

    @pl.when(place > 0)
    def _():
        rim_copy.wait_recv()
        conv_rows[0:RIM, :] = rim[...]

    @pl.when(place == 0)
    def _():
        conv_rows[0:RIM, :] = jnp.zeros((RIM, width), BF16)

    own_cols = pl.ds(pl.multiple_of(me * width, width), width)
    taps = conv_taps[:, own_cols].astype(F32)
    tap_count = conv_taps.shape[0]

    @pl.loop(0, nblocks)
    def _(b):
        rows = rows_of(b, BLOCK)
        x = conv_rows[pl.ds(pl.multiple_of(b * BLOCK, RIM), BLOCK + RIM), :].astype(F32)
        mixed = None
        for j in range(tap_count):
            back = tap_count - 1 - j
            y = x if back == 0 else pltpu.roll(x, back, 0)
            y = y[RIM:] * taps[j : j + 1]
            mixed = y if mixed is None else mixed + y
        mix[rows, pl.ds(width, width)] = (proj[GATE_OUT, rows, :].astype(F32) * mixed).astype(BF16)

    for h in range(heads):
        running[h] = init_memory[h]
    running_log[0:PAD] = jnp.zeros((PAD, BLOCK), F32)

    def advance(total, peak, term_of):
        old_log = running_log[0:PAD]
        merged = jnp.maximum(total + old_log, peak)
        keep = jnp.exp(total + old_log - merged)
        add = jnp.exp(peak - merged)
        running_log[0:PAD] = merged
        for h in range(heads):
            running[h] = keep[h : h + 1] * running[h] + add[h : h + 1] * term_of(h)

    @pl.loop(0, place)
    def _(source):
        for c in seg_copies(place, source, 0):
            c.wait_recv()
        advance(
            got_log[source, PAD : 2 * PAD],
            got_log[source, 0:PAD],
            lambda h: got_memory[source, h].astype(F32),
        )

    @pl.loop(0, nblocks)
    def _(b):
        starts_log[b] = running_log[0:PAD]
        for h in range(heads):
            starts[b, h] = running[h].astype(BF16)
        advance(block_sum[b], block_peak[b], lambda h: terms[b, h])

    def read_block(b):
        rows = rows_of(b, BLOCK)
        columns = col_log[b]
        for h in range(heads):
            peak = peak_log[b, :, h : h + 1]
            carried_log = columns[:, h : h + 1] + starts_log[b, h : h + 1, 0:1]
            top = jnp.maximum(carried_log, peak)
            carried = jnp.dot(
                proj[QUERY, rows, head_cols(h)], starts[b, h], preferred_element_type=F32
            )
            out = jnp.exp(carried_log - top) * carried + jnp.exp(peak - top) * within[b, h]
            out = out * lax.rsqrt(jnp.mean(out * out, axis=1, keepdims=True) + EPSILON)
            gate = jax.nn.sigmoid(proj[OUT_GATE, rows, head_cols(h)].astype(F32))
            head = head_rows[pl.ds(first_head + h, 1), :]
            mix[rows, head_cols(h)] = (out * head * gate).astype(BF16)

    def part_copy(c):
        return pltpu.make_async_remote_copy(
            src_ref=part_send.at[c],
            dst_ref=part_got.at[c],
            send_sem=part_sem_send.at[c],
            recv_sem=part_sem_recv.at[c],
            device_id={"tp": other},
            device_id_type=MESH,
        )

    def partial_rows(index, c):
        return jnp.dot(
            mix[rows_of(index, half), :], out_w[:, rows_of(c, out_cols)], preferred_element_type=F32
        ).astype(BF16)

    @pl.loop(0, n_out)
    def _(step):
        read_block(other * n_out + step)

    for c in out_copies:
        c.wait()

    @pl.loop(0, n_out)
    def _(step):
        part_send[step] = partial_rows(other, step)
        read_block(me * n_out + step)
        part_copy(step).start()

    @pl.loop(0, n_out)
    def _(c):
        own = partial_rows(me, c)
        part_copy(c).wait_recv()
        total = own.astype(F32) + part_got[c].astype(F32)
        layer_out[:, rows_of(c, out_cols)] = total.astype(BF16)

    token_copy.wait_send()

    @pl.when(place + 1 < n_sp)
    def _():
        rim_copy.wait_send()

    for d in range(1, n_sp):

        @pl.when(place + d < n_sp)
        def _(d=d):
            for c in seg_copies(place + d, place, d - 1):
                c.wait_send()

    @pl.loop(0, n_out)
    def _(c):
        part_copy(c).wait_send()


def local(
    tokens,
    norm_gain,
    w_query,
    w_key,
    w_value,
    w_outgate,
    w_gatein,
    w_gateout,
    w_convin,
    w_igate,
    w_fgate,
    input_bias,
    forget_bias,
    forget_extra,
    init_memory,
    head_gain,
    conv_taps,
    out_memory,
    out_conv,
):
    heads, dh = init_memory.shape[1], init_memory.shape[2]
    half, features = tokens.shape[1], tokens.shape[2]
    rows = forget_extra.shape[1]
    width = w_query.shape[1]
    nblocks = rows // BLOCK
    n_sp = lax.axis_size("sp")
    vmem = pl.BlockSpec(memory_space=pltpu.VMEM)
    hbm = pl.BlockSpec(memory_space=pl.ANY)
    smem = pl.BlockSpec(memory_space=pltpu.SMEM)
    dma = pltpu.SemaphoreType.DMA
    n_seg = max(n_sp - 1, 1)
    n_out = half // BLOCK
    out_cols = features // n_out
    out = pl.pallas_call(
        functools.partial(kernel, n_sp),
        name="layer",
        out_shape=pltpu.VMEM((half, features), BF16),
        in_specs=[hbm, vmem] + [hbm] * 7 + [vmem] * 2 + [smem] * 2 + [vmem] * 4 + [hbm] * 2,
        out_specs=vmem,
        scratch_shapes=[
            pltpu.VMEM((2, half, features), BF16),
            pltpu.VMEM((1, features), F32),
            pltpu.VMEM((PAD, BLOCK), F32),
            pltpu.VMEM((features, BLOCK), BF16),
            pltpu.VMEM((rows, features), BF16),
            pltpu.VMEM((7, features, width), BF16),
            pltpu.VMEM((2 * width, features), BF16),
            pltpu.VMEM((7, rows, width), BF16),
            pltpu.VMEM((rows, BLOCK), F32),
            pltpu.VMEM((nblocks, 2 * PAD, BLOCK), F32),
            pltpu.VMEM((nblocks, BLOCK, BLOCK), F32),
            pltpu.VMEM((nblocks, PAD, BLOCK), F32),
            pltpu.VMEM((nblocks, PAD, BLOCK), F32),
            pltpu.VMEM((nblocks, heads, dh, dh), F32),
            pltpu.VMEM((nblocks, heads, BLOCK, dh), F32),
            pltpu.VMEM((nblocks, BLOCK, BLOCK), F32),
            pltpu.VMEM((heads, dh, dh), F32),
            pltpu.VMEM((2 * PAD, BLOCK), F32),
            pltpu.VMEM((nblocks, heads, dh, dh), BF16),
            pltpu.VMEM((nblocks, PAD, BLOCK), F32),
            pltpu.VMEM((heads, dh, dh), BF16),
            pltpu.VMEM((2 * PAD, BLOCK), F32),
            pltpu.VMEM((n_seg, heads, dh, dh), BF16),
            pltpu.VMEM((n_seg, 2 * PAD, BLOCK), F32),
            pltpu.VMEM((RIM + rows, width), BF16),
            pltpu.VMEM((RIM, width), BF16),
            pltpu.VMEM((rows, 2 * width), BF16),
            pltpu.VMEM((n_out, half, out_cols), BF16),
            pltpu.VMEM((n_out, half, out_cols), BF16),
            dma((1,)),
            dma((9,)),
            dma((2,)),
            dma((2, n_seg)),
            dma((2, n_seg)),
            dma((2,)),
            dma((n_out,)),
            dma((n_out,)),
        ],
        compiler_params=pltpu.CompilerParams(
            collective_id=0, has_side_effects=True, vmem_limit_bytes=60 * 1024 * 1024
        ),
    )(
        tokens[0],
        norm_gain.reshape(-1, BLOCK),
        w_key,
        w_value,
        w_gatein,
        w_convin,
        w_gateout,
        w_query,
        w_outgate,
        jnp.transpose(w_igate),
        jnp.transpose(w_fgate),
        input_bias,
        forget_bias,
        jnp.transpose(forget_extra[0]),
        init_memory[0],
        head_gain.reshape(-1, dh),
        conv_taps,
        out_memory,
        out_conv,
    )
    return out[None]


def solution(mesh):
    return jax.shard_map(
        local,
        mesh=mesh,
        in_specs=(
            P("fs", ("sp", "tp"), None),
            P(),
            P(None, "tp"),
            P(None, "tp"),
            P(None, "tp"),
            P(None, "tp"),
            P(None, "tp"),
            P(None, "tp"),
            P(None, "tp"),
            P(),
            P(),
            P(),
            P(),
            P("fs", "sp", "tp"),
            P("fs", "tp", None, None),
            P(),
            P(),
            P("tp", None),
            P("tp", None),
        ),
        out_specs=P("fs", ("sp", "tp"), None),
        check_vma=False,
    )
```

```python
import functools

import jax
import jax.numpy as jnp
from jax import lax
from jax.experimental import pallas as pl
from jax.experimental.pallas import tpu as pltpu
from jax.sharding import PartitionSpec as P

BLOCK = 128
EPSILON = 1e-06
LOWEST_LOG = -1e30
MESH = pl.DeviceIdType.MESH
F32 = jnp.float32
BF16 = jnp.bfloat16
PAD = 8
RIM = 16
NORM_ROWS = 64

KEY, VALUE, QUERY, GATE_IN, CONV_IN, GATE_OUT, OUT_GATE = range(7)


def kernel(
    n_sp,
    tokens,
    norm_gain,
    w_key,
    w_value,
    w_gatein,
    w_convin,
    w_gateout,
    w_query,
    w_outgate,
    w_igate,
    w_fgate,
    input_bias,
    forget_bias,
    extra,
    init_memory,
    head_gain,
    conv_taps,
    out_memory,
    out_conv,
    layer_out,
    tok,
    gain_row,
    head_rows,
    gate_w,
    normed,
    weights,
    out_w,
    proj,
    gate_pre,
    row_log,
    col_log,
    block_sum,
    block_peak,
    terms,
    within,
    peak_log,
    running,
    running_log,
    starts,
    starts_log,
    seg_memory,
    seg_log,
    got_memory,
    got_log,
    conv_rows,
    rim,
    mix,
    part_send,
    part_got,
    local_sem,
    weight_sem,
    token_sem,
    seg_send,
    seg_recv,
    rim_sem,
    part_sem_send,
    part_sem_recv,
):
    me = lax.axis_index("tp")
    other = 1 - me
    place = lax.axis_index("sp")
    half = tok.shape[1]
    total_rows = normed.shape[0]
    width = w_key.shape[1]
    heads = init_memory.shape[0]
    dh = init_memory.shape[1]
    nblocks = total_rows // BLOCK
    key_factor = dh ** (-0.5)
    out_width = layer_out.shape[1]
    n_out = half // BLOCK
    out_cols = out_width // n_out

    barrier = pltpu.get_barrier_semaphore()
    pl.semaphore_signal(barrier, inc=1, device_id={"tp": other}, device_id_type=MESH)
    for d in range(1, n_sp):
        pl.semaphore_signal(
            barrier, inc=1, device_id={"sp": lax.rem(place + d, n_sp)}, device_id_type=MESH
        )

    own_copy = pltpu.make_async_copy(tokens, tok.at[0], local_sem.at[0])
    own_copy.start()
    w_in = (w_key, w_value, w_query, w_gatein, w_convin, w_gateout, w_outgate)
    w_copies = [
        pltpu.make_async_copy(w, weights.at[s], weight_sem.at[s]) for s, w in enumerate(w_in)
    ]
    out_copies = [
        pltpu.make_async_copy(out_memory, out_w.at[pl.ds(0, width)], weight_sem.at[7]),
        pltpu.make_async_copy(out_conv, out_w.at[pl.ds(width, width)], weight_sem.at[8]),
    ]
    for c in w_copies[:2]:
        c.start()

    pl.semaphore_wait(barrier, n_sp)
    token_copy = pltpu.make_async_remote_copy(
        src_ref=tokens,
        dst_ref=tok.at[1],
        send_sem=token_sem.at[0],
        recv_sem=token_sem.at[1],
        device_id={"tp": other},
        device_id_type=MESH,
    )
    token_copy.start()

    gates = jnp.concatenate(
        [w_fgate[...], w_igate[...], jnp.zeros((BLOCK - 2 * PAD, w_igate.shape[1]), BF16)], axis=0
    )
    gate_w[...] = jnp.transpose(gates)
    for j in range(norm_gain.shape[0]):
        gain_row[:, j * BLOCK : (j + 1) * BLOCK] = norm_gain[j : j + 1].astype(F32)
    head_rows[...] = head_gain[...].astype(F32)
    own_copy.wait()
    for c in w_copies[2:] + out_copies:
        c.start()

    def rows_of(index, size):
        return pl.ds(pl.multiple_of(index * size, size), size)

    def normalize(slot, base):
        @pl.loop(0, half // NORM_ROWS)
        def _(c):
            x = tok[slot, rows_of(c, NORM_ROWS), :].astype(F32)
            scale = lax.rsqrt(jnp.mean(x * x, axis=-1, keepdims=True) + EPSILON)
            y = (x * scale) * gain_row[...]
            normed[pl.ds(pl.multiple_of(base + c * NORM_ROWS, NORM_ROWS), NORM_ROWS), :] = y.astype(
                BF16
            )

    def project(slot, rows):
        proj[slot, rows, :] = jnp.dot(
            normed[rows, :], weights[slot], preferred_element_type=F32
        ).astype(BF16)

    @pl.loop(0, 2)
    def _(step):
        index = lax.rem(me + step, 2)

        @pl.when(step == 1)
        def _():
            token_copy.wait_recv()

        normalize(step, index * half)
        rows = rows_of(index, half)
        gate_pre[rows, :] = jnp.dot(normed[rows, :], gate_w[...], preferred_element_type=F32)

        @pl.loop(KEY, VALUE + 1)
        def _(slot):
            @pl.when(step == 0)
            def _():
                pltpu.make_async_copy(w_key, weights.at[slot], weight_sem.at[slot]).wait()

            project(slot, rows)

    row_i = lax.broadcasted_iota(jnp.int32, (BLOCK, BLOCK), 0)
    col_i = lax.broadcasted_iota(jnp.int32, (BLOCK, BLOCK), 1)
    upper = jnp.where(row_i <= col_i, 1.0, 0.0).astype(F32)
    for h in range(heads):
        running[h] = jnp.zeros((dh, dh), F32)
    running_log[0:PAD] = jnp.full((PAD, BLOCK), LOWEST_LOG, F32)
    running_log[PAD : 2 * PAD] = jnp.zeros((PAD, BLOCK), F32)

    def head_cols(h):
        return slice(h * dh, (h + 1) * dh)

    first_head = me * heads
    to_front = lax.rem(PAD - first_head, PAD)
    lane_head = lax.broadcasted_iota(jnp.int32, (PAD, BLOCK), 0)
    bias_f = jnp.zeros((PAD, BLOCK), F32)
    bias_i = jnp.zeros((PAD, BLOCK), F32)
    for h in range(heads):
        bias_f = jnp.where(lane_head == h, forget_bias[first_head + h], bias_f)
        bias_i = jnp.where(lane_head == h, input_bias[first_head + h], bias_i)
    no_head = jnp.zeros((PAD - heads, BLOCK), F32)

    forget_rows, in_rows = [], []
    for b in range(nblocks):
        span = slice(b * BLOCK, (b + 1) * BLOCK)
        pre = jnp.transpose(gate_pre[span, :])
        v = pltpu.roll(pre[0:PAD], to_front, 0) + bias_f
        log_forget = jnp.minimum(v, 0.0) - jnp.log1p(jnp.exp(-jnp.abs(v)))
        forget_rows.append(log_forget + jnp.concatenate([extra[:, span], no_head], axis=0))
        in_rows.append(pltpu.roll(pre[PAD : 2 * PAD], to_front, 0) + bias_i)
    all_cumulative = jnp.dot(
        jnp.concatenate(forget_rows, axis=0),
        upper,
        precision=lax.Precision.HIGHEST,
        preferred_element_type=F32,
    )
    all_in = jnp.concatenate(in_rows, axis=0)
    all_total = jnp.broadcast_to(all_cumulative[:, BLOCK - 1 : BLOCK], all_in.shape)
    exponent = all_total - all_cumulative + all_in
    all_peak = jnp.broadcast_to(jnp.max(exponent, axis=1, keepdims=True), all_in.shape)
    key_weight = jnp.exp(exponent - all_peak)
    filler = jnp.zeros((BLOCK - 2 * PAD, BLOCK), F32)
    for b in range(nblocks):
        span = slice(b * PAD, (b + 1) * PAD)
        row_log[b, 0:PAD] = all_cumulative[span]
        row_log[b, PAD : 2 * PAD] = all_in[span]
        block_sum[b] = all_total[span]
        block_peak[b] = all_peak[span]
        col_log[b] = jnp.transpose(
            jnp.concatenate([all_cumulative[span], key_weight[span], filler], axis=0)
        )

    @pl.loop(0, nblocks, unroll=2)
    def _(b):
        rows = rows_of(b, BLOCK)
        columns = col_log[b]
        total, peak = block_sum[b], block_peak[b]
        old_log = running_log[0:PAD]
        merged = jnp.maximum(total + old_log, peak)
        keep = jnp.exp(total + old_log - merged)
        add = jnp.exp(peak - merged)
        running_log[0:PAD] = merged
        running_log[PAD : 2 * PAD] = running_log[PAD : 2 * PAD] + total
        for h in range(heads):
            k = proj[KEY, rows, head_cols(h)].astype(F32)
            wk = (columns[:, PAD + h : PAD + h + 1] * k * key_factor).astype(BF16)
            term = lax.dot_general(
                wk,
                proj[VALUE, rows, head_cols(h)],
                (((0,), (0,)), ((), ())),
                preferred_element_type=F32,
            )
            terms[b, h] = term
            running[h] = keep[h : h + 1] * running[h] + add[h : h + 1] * term

    for h in range(heads):
        seg_memory[h] = running[h].astype(BF16)
    seg_log[...] = running_log[...]

    def seg_copies(target, source, d):
        return [
            pltpu.make_async_remote_copy(
                src_ref=src,
                dst_ref=dst.at[source],
                send_sem=seg_send.at[which, d],
                recv_sem=seg_recv.at[which, source],
                device_id={"sp": target},
                device_id_type=MESH,
            )
            for which, (src, dst) in enumerate(((seg_memory, got_memory), (seg_log, got_log)))
        ]

    for d in range(1, n_sp):

        @pl.when(place + d < n_sp)
        def _(d=d):
            for c in seg_copies(place + d, place, d - 1):
                c.start()

    causal = col_i <= row_i

    def own_terms(b):
        rows = rows_of(b, BLOCK)
        columns = col_log[b]
        for h in range(heads):
            q = proj[QUERY, rows, head_cols(h)]
            k = proj[KEY, rows, head_cols(h)]
            scores = lax.dot_general(q, k, (((1,), (1,)), ((), ())), preferred_element_type=F32)
            pair = (columns[:, h : h + 1] - row_log[b, h : h + 1]) + row_log[
                b, PAD + h : PAD + h + 1
            ]
            pair = jnp.where(causal, pair, -jnp.inf)
            peak = jnp.max(pair, axis=1, keepdims=True)
            weighted = (jnp.exp(pair - peak) * (scores * key_factor)).astype(BF16)
            peak_log[b, :, h : h + 1] = peak
            within[b, h] = jnp.dot(
                weighted, proj[VALUE, rows, head_cols(h)], preferred_element_type=F32
            )

    def weight_wait(slot):
        pltpu.make_async_copy(w_key, weights.at[slot], weight_sem.at[slot]).wait()

    weight_wait(QUERY)

    @pl.loop(0, 2)
    def _(index):
        project(QUERY, rows_of(index, half))

    per_job = nblocks // 8

    def finish(slots):
        @pl.loop(2 * slots[0], 2 * slots[1])
        def _(job):
            slot = job // 2
            index = lax.rem(job, 2)

            @pl.when(index == 0)
            def _():
                weight_wait(slot)

            for i in range(per_job):
                own_terms((job - 2 * GATE_IN) * per_job + i)
            project(slot, rows_of(index, half))

    finish((GATE_IN, CONV_IN + 1))

    @pl.loop(0, nblocks)
    def _(b):
        rows = rows_of(b, BLOCK)
        product = proj[GATE_IN, rows, :].astype(F32) * proj[CONV_IN, rows, :].astype(F32)
        conv_rows[pl.ds(pl.multiple_of(RIM + b * BLOCK, RIM), BLOCK), :] = product.astype(BF16)

    next_place = lax.rem(place + 1, n_sp)
    rim_copy = pltpu.make_async_remote_copy(
        src_ref=conv_rows.at[pl.ds(total_rows, RIM)],
        dst_ref=rim,
        send_sem=rim_sem.at[0],
        recv_sem=rim_sem.at[1],
        device_id={"sp": next_place},
        device_id_type=MESH,
    )

    @pl.when(place + 1 < n_sp)
    def _():
        rim_copy.start()

    finish((GATE_OUT, OUT_GATE + 1))

    @pl.when(place > 0)
    def _():
        rim_copy.wait_recv()
        conv_rows[0:RIM, :] = rim[...]

    @pl.when(place == 0)
    def _():
        conv_rows[0:RIM, :] = jnp.zeros((RIM, width), BF16)

    own_cols = pl.ds(pl.multiple_of(me * width, width), width)
    taps = conv_taps[:, own_cols].astype(F32)
    tap_count = conv_taps.shape[0]

    @pl.loop(0, nblocks)
    def _(b):
        rows = rows_of(b, BLOCK)
        x = conv_rows[pl.ds(pl.multiple_of(b * BLOCK, RIM), BLOCK + RIM), :].astype(F32)
        mixed = None
        for j in range(tap_count):
            back = tap_count - 1 - j
            y = x if back == 0 else pltpu.roll(x, back, 0)
            y = y[RIM:] * taps[j : j + 1]
            mixed = y if mixed is None else mixed + y
        mix[rows, pl.ds(width, width)] = (proj[GATE_OUT, rows, :].astype(F32) * mixed).astype(BF16)

    for h in range(heads):
        running[h] = init_memory[h]
    running_log[0:PAD] = jnp.zeros((PAD, BLOCK), F32)

    def advance(total, peak, term_of):
        old_log = running_log[0:PAD]
        merged = jnp.maximum(total + old_log, peak)
        keep = jnp.exp(total + old_log - merged)
        add = jnp.exp(peak - merged)
        running_log[0:PAD] = merged
        for h in range(heads):
            running[h] = keep[h : h + 1] * running[h] + add[h : h + 1] * term_of(h)

    @pl.loop(0, place)
    def _(source):
        for c in seg_copies(place, source, 0):
            c.wait_recv()
        advance(
            got_log[source, PAD : 2 * PAD],
            got_log[source, 0:PAD],
            lambda h: got_memory[source, h].astype(F32),
        )

    @pl.loop(0, nblocks)
    def _(b):
        starts_log[b] = running_log[0:PAD]
        for h in range(heads):
            starts[b, h] = running[h].astype(BF16)
        advance(block_sum[b], block_peak[b], lambda h: terms[b, h])

    def read_block(b):
        rows = rows_of(b, BLOCK)
        columns = col_log[b]
        for h in range(heads):
            peak = peak_log[b, :, h : h + 1]
            carried_log = columns[:, h : h + 1] + starts_log[b, h : h + 1, 0:1]
            top = jnp.maximum(carried_log, peak)
            carried = jnp.dot(
                proj[QUERY, rows, head_cols(h)], starts[b, h], preferred_element_type=F32
            )
            out = jnp.exp(carried_log - top) * carried + jnp.exp(peak - top) * within[b, h]
            out = out * lax.rsqrt(jnp.mean(out * out, axis=1, keepdims=True) + EPSILON)
            gate = jax.nn.sigmoid(proj[OUT_GATE, rows, head_cols(h)].astype(F32))
            head = head_rows[pl.ds(first_head + h, 1), :]
            mix[rows, head_cols(h)] = (out * head * gate).astype(BF16)

    def part_copy(c):
        return pltpu.make_async_remote_copy(
            src_ref=part_send.at[c],
            dst_ref=part_got.at[c],
            send_sem=part_sem_send.at[c],
            recv_sem=part_sem_recv.at[c],
            device_id={"tp": other},
            device_id_type=MESH,
        )

    def partial_rows(index, c):
        return jnp.dot(
            mix[rows_of(index, half), :], out_w[:, rows_of(c, out_cols)], preferred_element_type=F32
        ).astype(BF16)

    @pl.loop(0, n_out)
    def _(step):
        read_block(other * n_out + step)

    for c in out_copies:
        c.wait()

    @pl.loop(0, n_out)
    def _(step):
        part_send[step] = partial_rows(other, step)
        read_block(me * n_out + step)
        part_copy(step).start()

    @pl.loop(0, n_out)
    def _(c):
        own = partial_rows(me, c)
        part_copy(c).wait_recv()
        total = own.astype(F32) + part_got[c].astype(F32)
        layer_out[:, rows_of(c, out_cols)] = total.astype(BF16)

    token_copy.wait_send()

    @pl.when(place + 1 < n_sp)
    def _():
        rim_copy.wait_send()

    for d in range(1, n_sp):

        @pl.when(place + d < n_sp)
        def _(d=d):
            for c in seg_copies(place + d, place, d - 1):
                c.wait_send()

    @pl.loop(0, n_out)
    def _(c):
        part_copy(c).wait_send()


def local(
    tokens,
    norm_gain,
    w_query,
    w_key,
    w_value,
    w_outgate,
    w_gatein,
    w_gateout,
    w_convin,
    w_igate,
    w_fgate,
    input_bias,
    forget_bias,
    forget_extra,
    init_memory,
    head_gain,
    conv_taps,
    out_memory,
    out_conv,
):
    heads, dh = init_memory.shape[1], init_memory.shape[2]
    half, features = tokens.shape[1], tokens.shape[2]
    rows = forget_extra.shape[1]
    width = w_query.shape[1]
    nblocks = rows // BLOCK
    n_sp = lax.axis_size("sp")
    vmem = pl.BlockSpec(memory_space=pltpu.VMEM)
    hbm = pl.BlockSpec(memory_space=pl.ANY)
    smem = pl.BlockSpec(memory_space=pltpu.SMEM)
    dma = pltpu.SemaphoreType.DMA
    n_seg = max(n_sp - 1, 1)
    n_out = half // BLOCK
    out_cols = features // n_out
    out = pl.pallas_call(
        functools.partial(kernel, n_sp),
        name="layer",
        out_shape=pltpu.VMEM((half, features), BF16),
        in_specs=[hbm, vmem] + [hbm] * 7 + [vmem] * 2 + [smem] * 2 + [vmem] * 4 + [hbm] * 2,
        out_specs=vmem,
        scratch_shapes=[
            pltpu.VMEM((2, half, features), BF16),
            pltpu.VMEM((1, features), F32),
            pltpu.VMEM((PAD, BLOCK), F32),
            pltpu.VMEM((features, BLOCK), BF16),
            pltpu.VMEM((rows, features), BF16),
            pltpu.VMEM((7, features, width), BF16),
            pltpu.VMEM((2 * width, features), BF16),
            pltpu.VMEM((7, rows, width), BF16),
            pltpu.VMEM((rows, BLOCK), F32),
            pltpu.VMEM((nblocks, 2 * PAD, BLOCK), F32),
            pltpu.VMEM((nblocks, BLOCK, BLOCK), F32),
            pltpu.VMEM((nblocks, PAD, BLOCK), F32),
            pltpu.VMEM((nblocks, PAD, BLOCK), F32),
            pltpu.VMEM((nblocks, heads, dh, dh), F32),
            pltpu.VMEM((nblocks, heads, BLOCK, dh), F32),
            pltpu.VMEM((nblocks, BLOCK, BLOCK), F32),
            pltpu.VMEM((heads, dh, dh), F32),
            pltpu.VMEM((2 * PAD, BLOCK), F32),
            pltpu.VMEM((nblocks, heads, dh, dh), BF16),
            pltpu.VMEM((nblocks, PAD, BLOCK), F32),
            pltpu.VMEM((heads, dh, dh), BF16),
            pltpu.VMEM((2 * PAD, BLOCK), F32),
            pltpu.VMEM((n_seg, heads, dh, dh), BF16),
            pltpu.VMEM((n_seg, 2 * PAD, BLOCK), F32),
            pltpu.VMEM((RIM + rows, width), BF16),
            pltpu.VMEM((RIM, width), BF16),
            pltpu.VMEM((rows, 2 * width), BF16),
            pltpu.VMEM((n_out, half, out_cols), BF16),
            pltpu.VMEM((n_out, half, out_cols), BF16),
            dma((1,)),
            dma((9,)),
            dma((2,)),
            dma((2, n_seg)),
            dma((2, n_seg)),
            dma((2,)),
            dma((n_out,)),
            dma((n_out,)),
        ],
        compiler_params=pltpu.CompilerParams(
            collective_id=0, has_side_effects=True, vmem_limit_bytes=60 * 1024 * 1024
        ),
    )(
        tokens[0],
        norm_gain.reshape(-1, BLOCK),
        w_key,
        w_value,
        w_gatein,
        w_convin,
        w_gateout,
        w_query,
        w_outgate,
        jnp.transpose(w_igate),
        jnp.transpose(w_fgate),
        input_bias,
        forget_bias,
        jnp.transpose(forget_extra[0]),
        init_memory[0],
        head_gain.reshape(-1, dh),
        conv_taps,
        out_memory,
        out_conv,
    )
    return out[None]


def solution(mesh):
    return jax.shard_map(
        local,
        mesh=mesh,
        in_specs=(
            P("fs", ("sp", "tp"), None),
            P(),
            P(None, "tp"),
            P(None, "tp"),
            P(None, "tp"),
            P(None, "tp"),
            P(None, "tp"),
            P(None, "tp"),
            P(None, "tp"),
            P(),
            P(),
            P(),
            P(),
            P("fs", "sp", "tp"),
            P("fs", "tp", None, None),
            P(),
            P(),
            P("tp", None),
            P("tp", None),
        ),
        out_specs=P("fs", ("sp", "tp"), None),
        check_vma=False,
    )
```
